32 devices in a mesh: sp: 8 (over z, core), tp: 4 (over y, x).
Axes of the slice: x: 2, y: 2, z: 4, core: 2. Of those that a mesh axis runs over, the one named last changes fastest.
Arguments:
- receptance: bfloat16 [2048, 4096], P('sp', 'tp'), may hold values from -6 to 6
- key_vectors: bfloat16 [2048, 4096], P('sp', 'tp'), may hold values from -13 to 13
- value_vectors: bfloat16 [2048, 4096], P('sp', 'tp'), may hold values from -6 to 6
- decay_logits: bfloat16 [2048, 4096], P('sp', 'tp'), may hold values from -20 to 2
- rate_logits: bfloat16 [2048, 4096], P('sp', 'tp'), may hold values from -8 to 4
- gate_logits: bfloat16 [2048, 4096], P('sp', 'tp'), may hold values from -6 to 6
- group_gain: float32 [4096], P('tp'), may hold values from 0.1 to 1.9
- residual: bfloat16 [2048, 4096], P('sp', 'tp'), may hold values from -24 to 24
- mixer_out: bfloat16 [4096, 4096], P(None, 'tp'), may hold values from -0.09375 to 0.09375
- norm_gain: float32 [4096], P('tp'), may hold values from 0.1 to 1.9
- expert_ids: int32 [2048, 2], P('sp'), may hold values from 0 to 7, as said below
- route_weight: float32 [2048, 2], P('sp'), may hold values from 0.25 to 1
- expert_gate: bfloat16 [8, 4096, 1024], P('sp', 'tp'), may hold values from -0.09375 to 0.09375
- expert_up: bfloat16 [8, 4096, 1024], P('sp', 'tp'), may hold values from -0.09375 to 0.09375
- expert_down: bfloat16 [8, 1024, 4096], P('sp', None, 'tp'), may hold values from -0.1875 to 0.1875
Outputs:
- updated: bfloat16 [2048, 4096], P('sp', 'tp')
The draws below stay inside these ranges and needn't reach their ends.
Inputs may be any that keep to these rules, and one draw needn't show every extreme that they name: `expert_ids`: the experts of a row are different and lie in one group of 2 consecutive experts. In the rows of one index of sp (aligned blocks of 256 rows) no expert is named by more than 128 rows, and in every such block some expert is named by exactly 128 rows.
All inputs are finite; a program needn't handle non-finite values.
Results may differ from the reference program's by a relative error of at most 0.013.
Values may be sent and summed in bfloat16 or wider, within the bound.
A program may use at most 128 MiB of HBM per device.

```python
import math
import jax
import jax.numpy as jnp
from jax import lax

D = 4096
WIDTH = 4096
HEAD = 64
HEADS = 64
FF = 1024
GROUPS = 4
TOP = 2
TOK_SP = 256
EXPERTS = 8
GROUP_EXPERTS = 2
CAP = 128
SLOTS = 1024
TOKENS = 2048
CUTS = 4
DBLK = 1024
N_SP = 8


def fast_heads(key, count):
    order = jax.random.permutation(jax.random.fold_in(key, 7101), HEADS)
    return order < count


def draw_decay_logits(key, part):
    flags = fast_heads(key, HEADS // 2)
    noise = 0.6 * jnp.clip(jax.random.normal(jax.random.fold_in(key, 2), (TOKENS, WIDTH), jnp.float32), -3.0, 3.0)
    per_head = jnp.where(flags, math.log(1.0 / 16.0), math.log(0.8 / TOKENS))
    base = jnp.repeat(per_head, HEAD)
    channel = 0.3 * jnp.clip(jax.random.normal(jax.random.fold_in(key, 3), (WIDTH,), jnp.float32), -3.0, 3.0)
    halves = TOKENS // (TOK_SP // 2)
    drift = jax.random.uniform(jax.random.fold_in(key, 4), (halves, 1), jnp.float32, -1.1, 1.1)
    drift = jnp.repeat(drift, TOK_SP // 2, axis=0)
    log_rate = jnp.minimum(base[None, :] + channel[None, :] + drift + noise, -0.7)
    shifted = log_rate + 0.5
    return (shifted - jnp.log1p(-jnp.exp(shifted))).astype(jnp.bfloat16)


def draw_rate_logits(key, part):
    flags = fast_heads(key, HEADS // 2)
    spread = 0.7 * jnp.clip(jax.random.normal(jax.random.fold_in(key, 5), (TOKENS, WIDTH), jnp.float32), -2.4, 2.4)
    mixed_channels = jax.random.bernoulli(jax.random.fold_in(key, 6), 0.5, (WIDTH,))
    strong = jnp.logical_or(jnp.repeat(flags, HEAD), mixed_channels)
    centre = jnp.where(strong, 2.3, -6.0)
    width_scale = jnp.where(strong, 1.0, 0.5)
    return (centre[None, :] + width_scale[None, :] * spread).astype(jnp.bfloat16)


def draw_key_vectors(key, part):
    direction = jnp.clip(jax.random.normal(jax.random.fold_in(key, 21), (HEADS, HEAD), jnp.float32), -3.0, 3.0)
    along = 1.0 + 0.4 * jnp.clip(jax.random.normal(jax.random.fold_in(key, 22), (TOKENS, HEADS), jnp.float32), -2.0, 2.0)
    rough = jnp.clip(jax.random.normal(jax.random.fold_in(key, 23), (TOKENS, HEADS, HEAD), jnp.float32), -4.0, 4.0)
    keys = 1.5 * along[:, :, None] * direction[None, :, :] + rough
    return keys.reshape(TOKENS, WIDTH).astype(jnp.bfloat16)


def draw_residual(key, part):
    column_blocks = max(D // 128, 1)
    scales = jnp.exp(jax.random.uniform(jax.random.fold_in(key, 11), (column_blocks,), jnp.float32, math.log(0.4), math.log(2.5)))
    scales = jnp.repeat(scales, D // column_blocks)
    base = jnp.clip(jax.random.normal(jax.random.fold_in(key, 12), (TOKENS, D), jnp.float32), -5.0, 5.0)
    return (base * scales[None, :]).astype(jnp.bfloat16)


def draw_expert_ids(key, part):
    anchor = jax.random.fold_in(key, 9001)
    full_group = jax.random.randint(jax.random.fold_in(anchor, 1), (), 0, GROUPS)
    full_lead = jax.random.randint(jax.random.fold_in(anchor, 2), (), 0, GROUP_EXPERTS)
    block_keys = jax.random.split(jax.random.fold_in(anchor, 3), TOKENS // TOK_SP)
    spots = jnp.arange(GROUPS, dtype=jnp.int32)
    others_width = max(GROUP_EXPERTS - 1, 1)

    def one_block(block_key):
        keys_here = jax.random.split(block_key, 5)
        order = jax.random.permutation(keys_here[0], TOK_SP).astype(jnp.int32)
        held = jax.random.randint(keys_here[1], (), CAP, TOK_SP // 2 + 1)
        shift = jax.random.randint(keys_here[2], (), 0, GROUPS - 1)
        leads = jax.random.randint(keys_here[3], (GROUPS,), 0, GROUP_EXPERTS)
        leads = jnp.where(spots == full_group, full_lead, leads)
        shuffles = jax.vmap(lambda subkey: jax.random.permutation(subkey, others_width))(jax.random.split(keys_here[4], GROUPS)).astype(jnp.int32)
        in_full = order < held
        others = order - held
        group = jnp.where(in_full, full_group, (full_group + 1 + (others + shift) % (GROUPS - 1)) % GROUPS)
        rank = jnp.where(in_full, order, others // (GROUPS - 1))
        lead = leads[group]
        shuffle_rows = shuffles[group]

        def other_expert(position):
            pick = jnp.take_along_axis(shuffle_rows, (position % others_width)[:, None], axis=1)[:, 0]
            return (lead + 1 + pick) % GROUP_EXPERTS
        early = rank < CAP
        late_pos = CAP + 2 * (rank - CAP)
        first_pick = jnp.where(early, lead, other_expert(late_pos))
        second_pick = jnp.where(early, other_expert(rank), other_expert(late_pos + 1))
        return jnp.stack([group * GROUP_EXPERTS + first_pick, group * GROUP_EXPERTS + second_pick], axis=1)
    chosen = jax.vmap(one_block)(block_keys)
    return chosen.reshape(TOKENS, TOP).astype(jnp.int32)


def block_levels(own_key, extent, pieces, least, top_value):
    def one(dim, parts):
        steps = jax.random.uniform(jax.random.fold_in(jax.random.fold_in(own_key, 6), dim), (parts,), jnp.float32, least / len(pieces), top_value / len(pieces))
        return jnp.repeat(jnp.exp(steps), extent[dim] // parts).reshape((-1,) + (1,) * (len(extent) - dim - 1))

    loudness = one(*pieces[0])
    for cut in pieces[1:]:
        loudness = loudness * one(*cut)
    return loudness


def normal_values(key, dims, width, bound, cuts=(), kind=jnp.bfloat16):
    values = jax.random.normal(key, dims, jnp.float32) * width
    if len(cuts) > 0:
        values = block_levels(key, dims, cuts, -0.22, 0.18) * values
    return jnp.clip(values, min=-bound, max=bound).astype(kind)


def setup_inputs(seed: int = 0) -> dict:
    key_list = jax.random.split(jax.random.key(seed), 16)
    return {
        "receptance": normal_values(key_list[0], (TOKENS, WIDTH), 1.0, 6.0, ((0, 8), (1, 4))),
        "key_vectors": draw_key_vectors(jax.random.fold_in(key_list[15], 71), 0),
        "value_vectors": normal_values(key_list[2], (TOKENS, WIDTH), 1.0, 6.0, ((0, 8), (1, 4))),
        "decay_logits": draw_decay_logits(jax.random.fold_in(key_list[15], 71), 0),
        "rate_logits": draw_rate_logits(jax.random.fold_in(key_list[15], 71), 0),
        "gate_logits": normal_values(key_list[5], (TOKENS, WIDTH), 1.5, 6.0, ((0, 8), (1, 4))),
        "group_gain": jnp.clip(1.0 + 0.18 * jax.random.normal(key_list[6], (WIDTH,), jnp.float32), 0.1, 1.9),
        "residual": draw_residual(jax.random.fold_in(key_list[15], 71), 0),
        "mixer_out": normal_values(key_list[8], (WIDTH, D), WIDTH ** -0.5, 0.09375, ((1, 4),)),
        "norm_gain": jnp.clip(1.0 + 0.18 * jax.random.normal(key_list[9], (D,), jnp.float32), 0.1, 1.9),
        "expert_ids": draw_expert_ids(jax.random.fold_in(key_list[15], 71), 0),
        "route_weight": jnp.clip(0.25 + 0.75 * jax.random.uniform(key_list[11], (TOKENS, TOP), jnp.float32) ** block_levels(key_list[11], (TOKENS, TOP), ((0, 8),), -0.2, 0.2), 0.25, 1.0),
        "expert_gate": normal_values(key_list[12], (EXPERTS, D, FF), D ** -0.5, 0.09375, ((0, 8), (1, 4))),
        "expert_up": normal_values(key_list[13], (EXPERTS, D, FF), D ** -0.5, 0.09375, ((0, 8), (1, 4))),
        "expert_down": normal_values(key_list[14], (EXPERTS, FF, D), FF ** -0.5, 0.1875, ((0, 8), (2, 4))),
    }


EPS_GROUP = 0.00064
EPS_NORM = 1e-06
HIGHEST = lax.Precision.HIGHEST

def by_heads(array):
    return array.astype(jnp.float32).reshape(array.shape[0], WIDTH // HEAD, HEAD)

def time_mix(receptance, key_vectors, value_vectors, decay_logits, rate_logits, gate_logits, group_gain):
    recept = by_heads(receptance)
    keyvec = by_heads(key_vectors)
    valvec = by_heads(value_vectors)
    decay = jnp.exp(-jnp.exp(-jax.nn.softplus(-by_heads(decay_logits)) - 0.5))
    unit_key = keyvec / jnp.sqrt(1.0 + lax.optimization_barrier(jnp.sum(keyvec * keyvec, axis=-1, keepdims=True)))
    correction = unit_key * jax.nn.sigmoid(by_heads(rate_logits))

    def advance(carried, inputs):
        recept_now, decay_now, key_now, value_now, unit_now, corr_now = inputs
        pulled = jnp.einsum('hij,hj->hi', carried, unit_now, precision=HIGHEST)
        carried = carried * decay_now[:, None, :] - pulled[:, :, None] * corr_now[:, None, :] + value_now[:, :, None] * key_now[:, None, :]
        return (carried, jnp.einsum('hij,hj->hi', carried, recept_now, precision=HIGHEST))
    initial = jnp.zeros((WIDTH // HEAD, HEAD, HEAD), jnp.float32)
    final_state, state_read = lax.scan(advance, initial, (recept, decay, keyvec, valvec, unit_key, correction))
    centred = state_read - lax.optimization_barrier(jnp.mean(state_read, axis=-1, keepdims=True))
    scaled = centred * lax.rsqrt(lax.optimization_barrier(jnp.mean(centred * centred, axis=-1, keepdims=True)) + EPS_GROUP)
    gated_out = scaled.reshape(TOKENS, WIDTH) * group_gain.astype(jnp.float32)[None, :] * jax.nn.sigmoid(gate_logits.astype(jnp.float32))
    return gated_out.astype(jnp.bfloat16)

def block_ranks(expert_ids):
    grouped = expert_ids.reshape(N_SP, TOK_SP * TOP)
    onehot = (grouped[:, :, None] == jnp.arange(EXPERTS, dtype=jnp.int32)[None, None, :]).astype(jnp.int32)
    earlier = jnp.cumsum(onehot, axis=1) - onehot
    return lax.optimization_barrier(jnp.sum(earlier * onehot, axis=2)).reshape(TOKENS, TOP).astype(jnp.int32)

def cut_product(chosen, matrix):
    rows_cut = chosen.astype(jnp.float32).reshape(chosen.shape[0], CUTS, DBLK)
    matrix_cut = matrix.astype(jnp.float32).reshape(CUTS, DBLK, matrix.shape[1])
    partials = jnp.einsum('scd,cdf->csf', rows_cut, matrix_cut)
    rounded = lax.optimization_barrier(partials.astype(jnp.bfloat16))
    return lax.optimization_barrier(jnp.sum(rounded.astype(jnp.float32), axis=0))

def reference(receptance, key_vectors, value_vectors, decay_logits, rate_logits, gate_logits, group_gain, residual, mixer_out, norm_gain, expert_ids, route_weight, expert_gate, expert_up, expert_down):
    mixed_rows = time_mix(receptance, key_vectors, value_vectors, decay_logits, rate_logits, gate_logits, group_gain)
    midway = (residual.astype(jnp.float32) + jnp.dot(mixed_rows, mixer_out, preferred_element_type=jnp.float32)).astype(jnp.bfloat16)
    midway_f = midway.astype(jnp.float32)
    inv_rms = lax.rsqrt(lax.optimization_barrier(jnp.mean(midway_f * midway_f, axis=1, keepdims=True)) + EPS_NORM)
    normed = (midway_f * norm_gain.astype(jnp.float32)[None, :] * inv_rms).astype(jnp.bfloat16)
    ranks = block_ranks(expert_ids)
    token_ids = jnp.arange(TOKENS, dtype=jnp.int32)
    within = ((token_ids // TOK_SP)[:, None] * CAP + ranks).astype(jnp.int32)
    owners = jnp.broadcast_to(token_ids[:, None], expert_ids.shape).astype(jnp.int32)
    slot_table = jnp.full((EXPERTS, SLOTS), TOKENS, jnp.int32).at[expert_ids, within].set(owners)
    slot_weight = jnp.zeros((EXPERTS, SLOTS), jnp.float32).at[expert_ids, within].set(route_weight.astype(jnp.float32))
    padded = jnp.concatenate([normed, jnp.zeros((1, D), jnp.bfloat16)], axis=0)

    def one_expert(running, inputs):
        table_row, weight_row, gate_mat, up_mat, down_mat = inputs
        chosen = padded[table_row]
        hidden = (jax.nn.silu(cut_product(chosen, gate_mat)) * cut_product(chosen, up_mat)).astype(jnp.bfloat16)
        result = jnp.dot(hidden, down_mat, preferred_element_type=jnp.float32).astype(jnp.bfloat16)
        running = running.at[table_row].add(result.astype(jnp.float32) * weight_row[:, None])
        return (running, None)
    routed, unused = lax.scan(one_expert, jnp.zeros((TOKENS + 1, D), jnp.float32), (slot_table, slot_weight, expert_gate, expert_up, expert_down))
    return (midway_f + routed[:TOKENS]).astype(jnp.bfloat16)
```

```python
import jax
import jax.numpy as jnp
from jax import lax
from jax.experimental import pallas as pl
from jax.experimental.pallas import tpu as pltpu
from jax.sharding import PartitionSpec as P

D = 4096
HEAD = 64
CHUNK = 128
EXP_HALF = 0.6065306597126334


EPS_GROUP = 0.00064
EPS_NORM = 1e-06


def split(x):
    hi = x.astype(jnp.bfloat16)
    lo = (x - hi.astype(jnp.float32)).astype(jnp.bfloat16)
    return hi, lo


def dot(a, b, dims):
    return lax.dot_general(a, b, (dims, ((), ())), preferred_element_type=jnp.float32)


NN = ((1,), (0,))
NT = ((1,), (1,))
TN = ((0,), (0,))


def dot3(a, b, dims=NN):
    return dot(a[0], b[0], dims) + (dot(a[0], b[1], dims) + dot(a[1], b[0], dims))


def dot2(a, b, dims=NN):
    return dot(a[0], b, dims) + dot(a[1], b, dims)


def sigmoid(x):
    return 1.0 / (1.0 + jnp.exp(-x))


def mix_kernel(r_ref, k_ref, v_ref, d_ref, a_ref, out_ref, state_ref):
    tokens = r_ref.shape[0]
    chunks = tokens // CHUNK
    row = lax.broadcasted_iota(jnp.int32, (CHUNK, CHUNK), 0)
    col = lax.broadcasted_iota(jnp.int32, (CHUNK, CHUNK), 1)
    strict = col < row
    causal = col <= row
    eye = jnp.where(col == row, 1.0, 0.0)
    ones_lower = jnp.where(causal, 1.0, 0.0).astype(jnp.bfloat16)
    low = lax.broadcasted_iota(jnp.int32, (CHUNK, 2 * HEAD), 1) < HEAD

    work = []
    for chunk in range(chunks):
        rows = pl.ds(chunk * CHUNK, CHUNK)
        recept = r_ref[rows, :].astype(jnp.float32)
        keyvec = k_ref[rows, :].astype(jnp.float32)
        logdec = -EXP_HALF * sigmoid(d_ref[rows, :].astype(jnp.float32))
        first, second = split(logdec)
        third = (logdec - first.astype(jnp.float32) - second.astype(jnp.float32)).astype(jnp.bfloat16)
        cum_in = dot(ones_lower, first, NN) + (
            dot(ones_lower, second, NN) + dot(ones_lower, third, NN)
        )
        cum_end = cum_in[CHUNK - 1 :, :]
        squares = keyvec * keyvec
        norms = jnp.where(
            low,
            jnp.sum(squares[:, :HEAD], axis=1, keepdims=True),
            jnp.sum(squares[:, HEAD:], axis=1, keepdims=True),
        )
        unit_key = keyvec * lax.rsqrt(1.0 + norms)
        correction = unit_key * sigmoid(a_ref[rows, :].astype(jnp.float32))
        growth = jnp.exp(-cum_in)
        tail = jnp.exp(cum_end - cum_in)
        r_scaled = recept * jnp.exp(cum_in)
        u_scaled = unit_key * jnp.exp(cum_in - logdec)
        queries = split(jnp.concatenate([u_scaled, r_scaled], axis=0))
        sources = split(jnp.concatenate([keyvec * growth, correction * growth], axis=0))
        tails = split(jnp.concatenate([keyvec * tail, -(correction * tail)], axis=0))
        keep = jnp.broadcast_to(jnp.exp(cum_end), (2 * HEAD, 2 * HEAD)).T
        values = v_ref[rows, :]
        for head in range(2):
            lanes = slice(head * HEAD, (head + 1) * HEAD)
            query = tuple(q[:, lanes] for q in queries)
            source = tuple(s[:, lanes] for s in sources)
            scores = dot3(query, source, NT)
            work.append(
                dict(
                    head=head,
                    chunk=chunk,
                    query=query,
                    tail=tuple(t[:, lanes] for t in tails),
                    keep=keep[lanes, :],
                    value=jnp.concatenate(
                        [values[:, lanes], jnp.zeros((CHUNK, HEAD), jnp.bfloat16)], axis=1
                    ),
                    key_both=split(
                        jnp.concatenate(
                            [
                                jnp.where(strict, scores[:CHUNK, :CHUNK], 0.0),
                                jnp.where(causal, scores[CHUNK:, :CHUNK], 0.0),
                            ],
                            axis=0,
                        )
                    ),
                    pull=jnp.where(strict, scores[:CHUNK, CHUNK:], 0.0),
                    corr_read=split(jnp.where(causal, scores[CHUNK:, CHUNK:], 0.0)),
                )
            )
    for item in work:
        item["inverse"] = eye - jnp.where(row // 2 == col // 2, item["pull"], 0.0)
        item["from_values"] = dot2(item["key_both"], item["value"])
    size = 2
    while size < CHUNK:
        joined = (row // (2 * size) == col // (2 * size)) & (row // size != col // size)
        halves = []
        for item in work:
            inverse = split(item["inverse"])
            between = split(jnp.where(joined, item["pull"], 0.0))
            halves.append((inverse, dot3(between, inverse)))
        for item, (inverse, half) in zip(work, halves):
            item["inverse"] = item["inverse"] - dot3(inverse, split(half))
        size *= 2
    key_row = lax.broadcasted_iota(jnp.int32, (HEAD, 2 * HEAD), 0)
    lane = lax.broadcasted_iota(jnp.int32, (HEAD, 2 * HEAD), 1)
    start = jnp.where(lane == key_row + HEAD, 1.0, 0.0)
    states = [start, start]
    for item in work:
        head = item["head"]
        state = states[head]
        from_start = dot3(item["query"], split(state)) + item["from_values"]
        pulled = dot3(split(item["inverse"]), split(from_start[:CHUNK]))
        pulled_parts = split(pulled)
        out_ref[pl.ds(item["chunk"] * CHUNK, CHUNK), pl.ds(head * 2 * HEAD, 2 * HEAD)] = (
            from_start[CHUNK:] - dot3(item["corr_read"], pulled_parts)
        )
        key_tail = tuple(t[:CHUNK] for t in item["tail"])
        corr_tail = tuple(t[CHUNK:] for t in item["tail"])
        states[head] = (
            item["keep"] * state
            + dot2(key_tail, item["value"], TN)
            + dot3(corr_tail, pulled_parts, TN)
        )
    for head in range(2):
        state_ref[pl.ds(head * HEAD, HEAD), :] = states[head].astype(jnp.bfloat16)


def read_kernel(place_ref, read_ref, maps_ref, gate_ref, gain_ref, out_ref):
    def one(step, carried):
        following = []
        for head in range(2):
            both = maps_ref[step, pl.ds(head * HEAD, HEAD), :]
            parts = split(carried[head])
            step_map = both[:, HEAD:]
            following.append(
                both[:, :HEAD].astype(jnp.float32)
                + dot(step_map, parts[0], NN)
                + dot(step_map, parts[1], NN)
            )
        return tuple(following)

    zero = jnp.zeros((HEAD, HEAD), jnp.float32)
    incoming = lax.fori_loop(0, place_ref[0], one, (zero, zero))
    scaled = []
    for head in range(2):
        both = read_ref[:, pl.ds(head * 2 * HEAD, 2 * HEAD)]
        state_read = both[:, :HEAD] + dot3(split(both[:, HEAD:]), split(incoming[head]))
        centred = state_read - jnp.mean(state_read, axis=1, keepdims=True)
        variance = jnp.mean(centred * centred, axis=1, keepdims=True)
        scaled.append(centred * lax.rsqrt(variance + EPS_GROUP))
    gated = (
        jnp.concatenate(scaled, axis=1)
        * gain_ref[...]
        * sigmoid(gate_ref[...].astype(jnp.float32))
    )
    out_ref[...] = gated.astype(jnp.bfloat16)


def time_mix(
    receptance, key_vectors, value_vectors, decay_logits, rate_logits, gate_logits, group_gain
):
    tokens_here, channels = receptance.shape
    pairs = channels // (2 * HEAD)
    wide = pl.BlockSpec((tokens_here, 2 * HEAD), lambda i: (0, i))
    double = pl.BlockSpec((tokens_here, 4 * HEAD), lambda i: (0, i))
    reads, states = pl.pallas_call(
        mix_kernel,
        grid=(pairs,),
        in_specs=[wide] * 5,
        out_specs=[double, pl.BlockSpec((2 * HEAD, 2 * HEAD), lambda i: (i, 0))],
        out_shape=[
            jax.ShapeDtypeStruct((tokens_here, 2 * channels), jnp.float32),
            jax.ShapeDtypeStruct((channels, 2 * HEAD), jnp.bfloat16),
        ],
        name="mix",
    )(receptance, key_vectors, value_vectors, decay_logits, rate_logits)
    maps = lax.all_gather(states, "sp")
    place = lax.axis_index("sp").astype(jnp.int32).reshape(1)
    return pl.pallas_call(
        read_kernel,
        grid=(pairs,),
        in_specs=[
            pl.BlockSpec(memory_space=pltpu.SMEM),
            double,
            pl.BlockSpec((maps.shape[0], 2 * HEAD, 2 * HEAD), lambda i: (0, i, 0)),
            wide,
            pl.BlockSpec((1, 2 * HEAD), lambda i: (0, i)),
        ],
        out_specs=wide,
        out_shape=jax.ShapeDtypeStruct((tokens_here, channels), jnp.bfloat16),
        name="read",
    )(place, reads, maps, gate_logits, group_gain.reshape(1, channels))


def local(
    receptance,
    key_vectors,
    value_vectors,
    decay_logits,
    rate_logits,
    gate_logits,
    group_gain,
    residual,
    mixer_out,
    norm_gain,
    expert_ids,
    route_weight,
    expert_gate,
    expert_up,
    expert_down,
):
    mixed_rows = time_mix(
        receptance, key_vectors, value_vectors, decay_logits, rate_logits, gate_logits, group_gain
    )
    tokens_here, features = residual.shape
    projected = jnp.dot(
        lax.all_gather(mixed_rows, "tp", axis=1, tiled=True),
        mixer_out,
        preferred_element_type=jnp.float32,
    )
    midway = (residual.astype(jnp.float32) + projected).astype(jnp.bfloat16)
    midway_f = midway.astype(jnp.float32)
    squares = lax.psum(jnp.sum(midway_f * midway_f, axis=1), "tp")
    inv_rms = lax.rsqrt(squares / D + EPS_NORM)
    normed = (midway_f * norm_gain[None, :] * inv_rms[:, None]).astype(jnp.bfloat16)
    routes = expert_ids.shape[1]
    experts_all = lax.axis_size("sp") * expert_gate.shape[0]
    capacity = 2 * tokens_here * routes // experts_all
    flat_ids = expert_ids.reshape(-1)
    onehot = (flat_ids[:, None] == jnp.arange(experts_all, dtype=jnp.int32)[None, :]).astype(
        jnp.int32
    )
    earlier_count = jnp.sum((jnp.cumsum(onehot, axis=0) - onehot) * onehot, axis=1)
    slot_of = flat_ids * capacity + earlier_count
    owner_token = jnp.arange(tokens_here * routes, dtype=jnp.int32) // routes
    slot_table = (
        jnp.full((experts_all * capacity,), tokens_here, jnp.int32).at[slot_of].set(owner_token)
    )
    padded = jnp.concatenate([normed, jnp.zeros((1, features), jnp.bfloat16)], axis=0)
    outgoing = padded[slot_table].reshape(experts_all, capacity, features)
    arrived = lax.all_to_all(outgoing, "sp", split_axis=0, concat_axis=0, tiled=True)
    arrived_rows = arrived.reshape(-1, features)
    paired = jnp.concatenate([expert_gate[0], expert_up[0]], axis=1)
    gate_up = lax.psum_scatter(
        jnp.dot(arrived_rows, paired, preferred_element_type=jnp.float32).astype(jnp.bfloat16),
        "tp",
        scatter_dimension=0,
        tiled=True,
    ).astype(jnp.float32)
    half_width = paired.shape[1] // 2
    hidden = (jax.nn.silu(gate_up[:, :half_width]) * gate_up[:, half_width:]).astype(jnp.bfloat16)
    expert_res = jnp.dot(
        lax.all_gather(hidden, "tp", axis=0, tiled=True),
        expert_down[0],
        preferred_element_type=jnp.float32,
    )
    returned = lax.all_to_all(
        expert_res.astype(jnp.bfloat16).reshape(-1, capacity, features),
        "sp",
        split_axis=0,
        concat_axis=0,
        tiled=True,
    )
    picked = (
        returned.reshape(-1, features)[slot_of]
        .astype(jnp.float32)
        .reshape(tokens_here, routes, features)
    )
    routed_sum = jnp.sum(picked * route_weight[:, :, None], axis=1)
    return (midway_f + routed_sum).astype(jnp.bfloat16)


def solution(mesh):
    placed = (
        P("sp", "tp"),
        P("sp", "tp"),
        P("sp", "tp"),
        P("sp", "tp"),
        P("sp", "tp"),
        P("sp", "tp"),
        P("tp"),
        P("sp", "tp"),
        P(None, "tp"),
        P("tp"),
        P("sp", None),
        P("sp", None),
        P("sp", "tp", None),
        P("sp", "tp", None),
        P("sp", None, "tp"),
    )
    return jax.shard_map(
        local, mesh=mesh, in_specs=placed, out_specs=P("sp", "tp"), check_vma=False
    )
```

```python
import jax
import jax.numpy as jnp
from jax import lax
from jax.experimental import pallas as pl
from jax.experimental.pallas import tpu as pltpu
from jax.sharding import PartitionSpec as P

D = 4096
HEAD = 64
CHUNK = 128
EXP_HALF = 0.6065306597126334


EPS_GROUP = 0.00064
EPS_NORM = 1e-06


def split(x):
    hi = x.astype(jnp.bfloat16)
    lo = (x - hi.astype(jnp.float32)).astype(jnp.bfloat16)
    return hi, lo


def dot(a, b, dims):
    return lax.dot_general(a, b, (dims, ((), ())), preferred_element_type=jnp.float32)


NN = ((1,), (0,))
NT = ((1,), (1,))
TN = ((0,), (0,))


def dot3(a, b, dims=NN):
    return dot(a[0], b[0], dims) + (dot(a[0], b[1], dims) + dot(a[1], b[0], dims))


def dot2(a, b, dims=NN):
    return dot(a[0], b, dims) + dot(a[1], b, dims)


def sigmoid(x):
    return 1.0 / (1.0 + jnp.exp(-x))


def mix_kernel(r_ref, k_ref, v_ref, d_ref, a_ref, out_ref, state_ref):
    tokens = r_ref.shape[0]
    chunks = tokens // CHUNK
    row = lax.broadcasted_iota(jnp.int32, (CHUNK, CHUNK), 0)
    col = lax.broadcasted_iota(jnp.int32, (CHUNK, CHUNK), 1)
    strict = col < row
    causal = col <= row
    eye = jnp.where(col == row, 1.0, 0.0)
    ones_lower = jnp.where(causal, 1.0, 0.0).astype(jnp.bfloat16)
    low = lax.broadcasted_iota(jnp.int32, (CHUNK, 2 * HEAD), 1) < HEAD

    work = []
    for chunk in range(chunks):
        rows = pl.ds(chunk * CHUNK, CHUNK)
        recept = r_ref[rows, :].astype(jnp.float32)
        keyvec = k_ref[rows, :].astype(jnp.float32)
        logdec = -EXP_HALF * sigmoid(d_ref[rows, :].astype(jnp.float32))
        first, second = split(logdec)
        third = (logdec - first.astype(jnp.float32) - second.astype(jnp.float32)).astype(jnp.bfloat16)
        cum_in = dot(ones_lower, first, NN) + (
            dot(ones_lower, second, NN) + dot(ones_lower, third, NN)
        )
        cum_end = cum_in[CHUNK - 1 :, :]
        squares = keyvec * keyvec
        norms = jnp.where(
            low,
            jnp.sum(squares[:, :HEAD], axis=1, keepdims=True),
            jnp.sum(squares[:, HEAD:], axis=1, keepdims=True),
        )
        unit_key = keyvec * lax.rsqrt(1.0 + norms)
        correction = unit_key * sigmoid(a_ref[rows, :].astype(jnp.float32))
        growth = jnp.exp(-cum_in)
        tail = jnp.exp(cum_end - cum_in)
        r_scaled = recept * jnp.exp(cum_in)
        u_scaled = unit_key * jnp.exp(cum_in - logdec)
        queries = split(jnp.concatenate([u_scaled, r_scaled], axis=0))
        sources = split(jnp.concatenate([keyvec * growth, correction * growth], axis=0))
        tails = split(jnp.concatenate([keyvec * tail, -(correction * tail)], axis=0))
        keep = jnp.broadcast_to(jnp.exp(cum_end), (2 * HEAD, 2 * HEAD)).T
        values = v_ref[rows, :]
        for head in range(2):
            lanes = slice(head * HEAD, (head + 1) * HEAD)
            query = tuple(q[:, lanes] for q in queries)
            source = tuple(s[:, lanes] for s in sources)
            scores = dot3(query, source, NT)
            work.append(
                dict(
                    head=head,
                    chunk=chunk,
                    query=query,
                    tail=tuple(t[:, lanes] for t in tails),
                    keep=keep[lanes, :],
                    value=jnp.concatenate(
                        [values[:, lanes], jnp.zeros((CHUNK, HEAD), jnp.bfloat16)], axis=1
                    ),
                    key_both=split(
                        jnp.concatenate(
                            [
                                jnp.where(strict, scores[:CHUNK, :CHUNK], 0.0),
                                jnp.where(causal, scores[CHUNK:, :CHUNK], 0.0),
                            ],
                            axis=0,
                        )
                    ),
                    pull=jnp.where(strict, scores[:CHUNK, CHUNK:], 0.0),
                    corr_read=split(jnp.where(causal, scores[CHUNK:, CHUNK:], 0.0)),
                )
            )
    for item in work:
        item["inverse"] = eye - jnp.where(row // 2 == col // 2, item["pull"], 0.0)
        item["from_values"] = dot2(item["key_both"], item["value"])
    size = 2
    while size < CHUNK:
        joined = (row // (2 * size) == col // (2 * size)) & (row // size != col // size)
        halves = []
        for item in work:
            inverse = split(item["inverse"])
            between = split(jnp.where(joined, item["pull"], 0.0))
            halves.append((inverse, dot3(between, inverse)))
        for item, (inverse, half) in zip(work, halves):
            item["inverse"] = item["inverse"] - dot3(inverse, split(half))
        size *= 2
    key_row = lax.broadcasted_iota(jnp.int32, (HEAD, 2 * HEAD), 0)
    lane = lax.broadcasted_iota(jnp.int32, (HEAD, 2 * HEAD), 1)
    start = jnp.where(lane == key_row + HEAD, 1.0, 0.0)
    states = [start, start]
    for item in work:
        head = item["head"]
        state = states[head]
        from_start = dot3(item["query"], split(state)) + item["from_values"]
        pulled = dot3(split(item["inverse"]), split(from_start[:CHUNK]))
        pulled_parts = split(pulled)
        out_ref[pl.ds(item["chunk"] * CHUNK, CHUNK), pl.ds(head * 2 * HEAD, 2 * HEAD)] = (
            from_start[CHUNK:] - dot3(item["corr_read"], pulled_parts)
        )
        key_tail = tuple(t[:CHUNK] for t in item["tail"])
        corr_tail = tuple(t[CHUNK:] for t in item["tail"])
        states[head] = (
            item["keep"] * state
            + dot2(key_tail, item["value"], TN)
            + dot3(corr_tail, pulled_parts, TN)
        )
    for head in range(2):
        state_ref[pl.ds(head * HEAD, HEAD), :] = states[head].astype(jnp.bfloat16)


def read_kernel(place_ref, read_ref, maps_ref, gate_ref, gain_ref, out_ref):
    def one(step, carried):
        following = []
        for head in range(2):
            both = maps_ref[step, pl.ds(head * HEAD, HEAD), :]
            parts = split(carried[head])
            step_map = both[:, HEAD:]
            following.append(
                both[:, :HEAD].astype(jnp.float32)
                + dot(step_map, parts[0], NN)
                + dot(step_map, parts[1], NN)
            )
        return tuple(following)

    zero = jnp.zeros((HEAD, HEAD), jnp.float32)
    incoming = lax.fori_loop(0, place_ref[0], one, (zero, zero))
    scaled = []
    for head in range(2):
        both = read_ref[:, pl.ds(head * 2 * HEAD, 2 * HEAD)]
        state_read = both[:, :HEAD] + dot3(split(both[:, HEAD:]), split(incoming[head]))
        centred = state_read - jnp.mean(state_read, axis=1, keepdims=True)
        variance = jnp.mean(centred * centred, axis=1, keepdims=True)
        scaled.append(centred * lax.rsqrt(variance + EPS_GROUP))
    gated = (
        jnp.concatenate(scaled, axis=1)
        * gain_ref[...]
        * sigmoid(gate_ref[...].astype(jnp.float32))
    )
    out_ref[...] = gated.astype(jnp.bfloat16)


def time_mix(
    receptance, key_vectors, value_vectors, decay_logits, rate_logits, gate_logits, group_gain
):
    tokens_here, channels = receptance.shape
    pairs = channels // (2 * HEAD)
    wide = pl.BlockSpec((tokens_here, 2 * HEAD), lambda i: (0, i))
    double = pl.BlockSpec((tokens_here, 4 * HEAD), lambda i: (0, i))
    reads, states = pl.pallas_call(
        mix_kernel,
        grid=(pairs,),
        in_specs=[wide] * 5,
        out_specs=[double, pl.BlockSpec((2 * HEAD, 2 * HEAD), lambda i: (i, 0))],
        out_shape=[
            jax.ShapeDtypeStruct((tokens_here, 2 * channels), jnp.float32),
            jax.ShapeDtypeStruct((channels, 2 * HEAD), jnp.bfloat16),
        ],
        name="mix",
    )(receptance, key_vectors, value_vectors, decay_logits, rate_logits)
    maps = lax.all_gather(states, "sp")
    place = lax.axis_index("sp").astype(jnp.int32).reshape(1)
    return pl.pallas_call(
        read_kernel,
        grid=(pairs,),
        in_specs=[
            pl.BlockSpec(memory_space=pltpu.SMEM),
            double,
            pl.BlockSpec((maps.shape[0], 2 * HEAD, 2 * HEAD), lambda i: (0, i, 0)),
            wide,
            pl.BlockSpec((1, 2 * HEAD), lambda i: (0, i)),
        ],
        out_specs=wide,
        out_shape=jax.ShapeDtypeStruct((tokens_here, channels), jnp.bfloat16),
        name="read",
    )(place, reads, maps, gate_logits, group_gain.reshape(1, channels))


def exchange(x, axis, shape, source, target, collective_id, name):
    def kernel(x_ref, out_ref, stage, send_sem, recv_sem, local_sem):
        n = lax.axis_size(axis)
        me = lax.axis_index(axis)
        peers = [lax.rem(me + step, n) for step in range(1, n)]
        barrier = pltpu.get_barrier_semaphore()
        for peer in peers:
            pl.semaphore_signal(
                barrier, inc=1, device_id={axis: peer}, device_id_type=pl.DeviceIdType.MESH
            )
        pl.semaphore_wait(barrier, n - 1)
        copies = []
        for step, peer in enumerate(peers):
            copy = pltpu.make_async_remote_copy(
                src_ref=source(x_ref, peer),
                dst_ref=target(out_ref, me),
                send_sem=send_sem.at[step],
                recv_sem=recv_sem.at[step],
                device_id={axis: peer},
                device_id_type=pl.DeviceIdType.MESH,
            )
            copy.start()
            copies.append(copy)
        own = pltpu.make_async_copy(source(x_ref, me), stage, local_sem)
        own.start()
        own.wait()
        own = pltpu.make_async_copy(stage, target(out_ref, me), local_sem)
        own.start()
        own.wait()
        for copy in copies:
            copy.wait()

    n = lax.axis_size(axis)
    return pl.pallas_call(
        kernel,
        in_specs=[pl.BlockSpec(memory_space=pl.ANY)],
        out_specs=pl.BlockSpec(memory_space=pl.ANY),
        out_shape=jax.ShapeDtypeStruct(shape, x.dtype),
        scratch_shapes=[
            pltpu.VMEM(x.shape[-2:], x.dtype),
            pltpu.SemaphoreType.DMA((n - 1,)),
            pltpu.SemaphoreType.DMA((n - 1,)),
            pltpu.SemaphoreType.DMA,
        ],
        compiler_params=pltpu.CompilerParams(collective_id=collective_id, has_side_effects=True),
        name=name,
    )(x)


def gather_columns(x, axis, collective_id):
    rows, columns = x.shape
    return exchange(
        x,
        axis,
        (rows, lax.axis_size(axis) * columns),
        lambda ref, peer: ref,
        lambda ref, me: ref.at[:, pl.ds(pl.multiple_of(me * columns, columns), columns)],
        collective_id,
        "gather_columns",
    )


def gather_rows(x, axis, collective_id):
    rows, columns = x.shape
    return exchange(
        x,
        axis,
        (lax.axis_size(axis) * rows, columns),
        lambda ref, peer: ref,
        lambda ref, me: ref.at[pl.ds(pl.multiple_of(me * rows, rows), rows), :],
        collective_id,
        "gather_rows",
    )


def swap_blocks(x, axis, collective_id):
    return exchange(
        x, axis, x.shape, lambda ref, peer: ref.at[peer], lambda ref, me: ref.at[me],
        collective_id, "swap_blocks",
    )


def local(
    receptance,
    key_vectors,
    value_vectors,
    decay_logits,
    rate_logits,
    gate_logits,
    group_gain,
    residual,
    mixer_out,
    norm_gain,
    expert_ids,
    route_weight,
    expert_gate,
    expert_up,
    expert_down,
):
    mixed_rows = time_mix(
        receptance, key_vectors, value_vectors, decay_logits, rate_logits, gate_logits, group_gain
    )
    tokens_here, features = residual.shape
    projected = jnp.dot(
        gather_columns(mixed_rows, "tp", 0),
        mixer_out,
        preferred_element_type=jnp.float32,
    )
    midway = (residual.astype(jnp.float32) + projected).astype(jnp.bfloat16)
    midway_f = midway.astype(jnp.float32)
    squares = lax.psum(jnp.sum(midway_f * midway_f, axis=1), "tp")
    inv_rms = lax.rsqrt(squares / D + EPS_NORM)
    normed = (midway_f * norm_gain[None, :] * inv_rms[:, None]).astype(jnp.bfloat16)
    routes = expert_ids.shape[1]
    experts_all = lax.axis_size("sp") * expert_gate.shape[0]
    capacity = 2 * tokens_here * routes // experts_all
    flat_ids = expert_ids.reshape(-1)
    onehot = (flat_ids[:, None] == jnp.arange(experts_all, dtype=jnp.int32)[None, :]).astype(
        jnp.int32
    )
    earlier_count = jnp.sum((jnp.cumsum(onehot, axis=0) - onehot) * onehot, axis=1)
    slot_of = flat_ids * capacity + earlier_count
    owner_token = jnp.arange(tokens_here * routes, dtype=jnp.int32) // routes
    slot_table = (
        jnp.full((experts_all * capacity,), tokens_here, jnp.int32).at[slot_of].set(owner_token)
    )
    padded = jnp.concatenate([normed, jnp.zeros((1, features), jnp.bfloat16)], axis=0)
    outgoing = padded[slot_table].reshape(experts_all, capacity, features)
    arrived = swap_blocks(outgoing, "sp", 2)
    arrived_rows = arrived.reshape(-1, features)
    paired = jnp.concatenate([expert_gate[0], expert_up[0]], axis=1)
    gate_up = lax.psum_scatter(
        jnp.dot(arrived_rows, paired, preferred_element_type=jnp.float32).astype(jnp.bfloat16),
        "tp",
        scatter_dimension=0,
        tiled=True,
    ).astype(jnp.float32)
    half_width = paired.shape[1] // 2
    hidden = (jax.nn.silu(gate_up[:, :half_width]) * gate_up[:, half_width:]).astype(jnp.bfloat16)
    expert_res = jnp.dot(
        gather_rows(hidden, "tp", 1),
        expert_down[0],
        preferred_element_type=jnp.float32,
    )
    returned = swap_blocks(
        expert_res.astype(jnp.bfloat16).reshape(-1, capacity, features), "sp", 3
    )
    picked = (
        returned.reshape(-1, features)[slot_of]
        .astype(jnp.float32)
        .reshape(tokens_here, routes, features)
    )
    routed_sum = jnp.sum(picked * route_weight[:, :, None], axis=1)
    return (midway_f + routed_sum).astype(jnp.bfloat16)


def solution(mesh):
    placed = (
        P("sp", "tp"),
        P("sp", "tp"),
        P("sp", "tp"),
        P("sp", "tp"),
        P("sp", "tp"),
        P("sp", "tp"),
        P("tp"),
        P("sp", "tp"),
        P(None, "tp"),
        P("tp"),
        P("sp", None),
        P("sp", None),
        P("sp", "tp", None),
        P("sp", "tp", None),
        P("sp", None, "tp"),
    )
    return jax.shard_map(
        local, mesh=mesh, in_specs=placed, out_specs=P("sp", "tp"), check_vma=False
    )
```
